512 devices in a mesh: sp: 64 (over z, y), tp: 8 (over x, core).
Axes of the slice: x: 4, y: 4, z: 16, core: 2. Of those that a mesh axis runs over, the one named last changes fastest.
Arguments:
- residual_signal: bfloat16 [16384, 2048], P('sp'), may hold values from -6 to 6
- reading_probe_preactivations: bfloat16 [16384, 1024], P('sp', 'tp'), may hold values from -6 to 6
- keep_switch_preactivations: bfloat16 [16384, 1024], P('sp', 'tp'), may hold values from -5.5 to 5.5
- written_entries: bfloat16 [16384, 1024], P('sp', 'tp'), may hold values from -6 to 6
- emission_switch_preactivations: bfloat16 [16384, 1024], P('sp', 'tp'), may hold values from -6 to 6
- additional_shrink_amount: float32 [16384, 1024], P('sp', 'tp'), may hold values from -0.7 to 0
- complement_of_floor: float32 [1024], P('tp'), may hold values from 6.1035156e-06 to 0.1
- per_group_rescaler: float32 [128], replicated, may hold values from 0.1 to 1.9
- emission_linear_map: bfloat16 [1024, 2048], P('tp'), may hold values from -0.1875 to 0.1875
- channel_layer_rescaler: float32 [2048], replicated, may hold values from 0.1 to 1.9
- expanding_linear_map: bfloat16 [2048, 8192], P('sp', 'tp'), may hold values from -0.125 to 0.125
- contracting_linear_map: bfloat16 [2048, 8192], P('sp', 'tp'), may hold values from -0.0625 to 0.0625
Outputs:
- layer_out: bfloat16 [16384, 2048], P('sp')
The draws below stay inside these ranges and needn't reach their ends.
All inputs are finite; a program needn't handle non-finite values.
Results may differ from the reference program's by a relative error of at most 0.006.
Values may be sent and summed in bfloat16 or wider, within the bound.
A program may use at most 64 MiB of HBM per device.

```python
import jax
import jax.numpy as jnp
from jax import lax

D = 2048
HEADS = 8
HEAD = 128
FF = 8192
BLOCK = 64
TOK_DEV = 256
MIX = 1024
TOKENS = 16384


def draw_complement_of_floor(key, part):
    pick_key = jax.random.fold_in(key, 11)
    fast_key = jax.random.fold_in(key, 12)
    slow_key = jax.random.fold_in(key, 13)
    share = 0.5
    quick = jax.random.bernoulli(pick_key, share, (MIX,))
    fast_gap = jnp.exp(jax.random.uniform(fast_key, (MIX,), jnp.float32, jnp.log(0.04), jnp.log(0.1)))
    slow_gap = 2.0 / TOKENS * jnp.exp(jax.random.uniform(slow_key, (MIX,), jnp.float32, jnp.log(0.05), 0.0))
    return jnp.where(quick, fast_gap, slow_gap).astype(jnp.float32)


def draw_keep_switch_preactivations(key, part):
    offset_key = jax.random.fold_in(key, 21)
    noise_key = jax.random.fold_in(key, 22)
    offsets = jax.random.uniform(offset_key, (TOKENS // TOK_DEV,), jnp.float32, -1.5, 1.5)
    shifts = jnp.repeat(offsets, TOK_DEV, total_repeat_length=TOKENS)[:, None]
    noise = jnp.clip(jax.random.normal(noise_key, (TOKENS, MIX), jnp.float32), -4.0, 4.0)
    return (noise + shifts).astype(jnp.bfloat16)


def draw_additional_shrink_amount(key, part):
    place_key = jax.random.fold_in(key, 31)
    value_key = jax.random.fold_in(key, 32)
    places = jax.random.randint(place_key, (3,), 0, TOKENS)
    rows = jnp.arange(TOKENS)
    struck = jnp.any(rows[:, None] == places[None, :], axis=1)
    values = jnp.log(jax.random.uniform(value_key, (TOKENS, MIX), jnp.float32, 0.5, 0.8))
    return jnp.where(struck[:, None], values, 0.0).astype(jnp.float32)


def steps_of(own_key, dims, shards, low, largest):
    level = 1.0
    for position, blocks in shards:
        steps = jax.random.uniform(jax.random.fold_in(jax.random.fold_in(own_key, 6), position), (blocks,), jnp.float32, low / len(shards), largest / len(shards))
        level = level * jnp.repeat(jnp.exp(steps), dims[position] // blocks).reshape((-1,) + (1,) * (len(dims) - 1 - position))
    return level


def centred(rng, shape, width, reach, shards=(), held_as=jnp.bfloat16):
    drawn = jax.random.normal(rng, shape, jnp.float32) * width
    if len(shards) > 0:
        drawn = steps_of(rng, shape, shards, -0.22, 0.18) * drawn
    return jnp.clip(drawn, min=-reach, max=reach).astype(held_as)


def setup_inputs(seed: int = 0) -> dict:
    arg_keys = jax.random.split(jax.random.key(seed), 13)
    return {
        "residual_signal": centred(arg_keys[0], (TOKENS, D), 1.0, 6.0, ((0, 64),)),
        "reading_probe_preactivations": centred(arg_keys[1], (TOKENS, MIX), 1.0, 6.0, ((0, 64), (1, 8))),
        "keep_switch_preactivations": draw_keep_switch_preactivations(jax.random.fold_in(arg_keys[12], 71), 0),
        "written_entries": centred(arg_keys[3], (TOKENS, MIX), 1.0, 6.0, ((0, 64), (1, 8))),
        "emission_switch_preactivations": centred(arg_keys[4], (TOKENS, MIX), 1.0, 6.0, ((0, 64), (1, 8))),
        "additional_shrink_amount": draw_additional_shrink_amount(jax.random.fold_in(arg_keys[12], 71), 0),
        "complement_of_floor": draw_complement_of_floor(jax.random.fold_in(arg_keys[12], 71), 0),
        "per_group_rescaler": jnp.clip(1.0 + 0.18 * jax.random.normal(arg_keys[7], (HEAD,), jnp.float32), 0.1, 1.9),
        "emission_linear_map": centred(arg_keys[8], (MIX, D), MIX ** -0.5, 0.1875, ((0, 8),)),
        "channel_layer_rescaler": jnp.clip(1.0 + 0.18 * jax.random.normal(arg_keys[9], (D,), jnp.float32), 0.1, 1.9),
        "expanding_linear_map": centred(arg_keys[10], (D, FF), D ** -0.5, 0.125, ((0, 64), (1, 8))),
        "contracting_linear_map": centred(arg_keys[11], (D, FF), FF ** -0.5, 0.0625, ((0, 64), (1, 8))),
    }


norm_eps = 1e-06
HIGH_ACCURACY = lax.Precision.HIGHEST

def block_step(state_matrix, inputs):
    query_block_rows, key_blk, logs_blk, value_block_rows = inputs
    cumulative_decay = jnp.cumsum(logs_blk, axis=1)
    carried_state = jnp.einsum('rlb,rbz->rlz', query_block_rows * jnp.exp(cumulative_decay), state_matrix, precision=HIGH_ACCURACY)
    spread = cumulative_decay[:, :, None, :] - cumulative_decay[:, None, :, :]
    places = jnp.arange(BLOCK)
    lower = places[:, None] >= places[None, :]
    decay = jnp.exp(jnp.where(lower[None, :, :, None], spread, -jnp.inf))
    scores = jnp.einsum('htk,hsk,htsk->hts', query_block_rows, key_blk, decay, precision=HIGH_ACCURACY)
    result = carried_state + jnp.einsum('hts,hsv->htv', scores, value_block_rows, precision=HIGH_ACCURACY)
    final_state = cumulative_decay[:, -1:, :]
    decayed_key_rows = key_blk * jnp.exp(final_state - cumulative_decay)
    state_matrix = jnp.exp(final_state[:, 0, :])[..., None] * state_matrix + jnp.einsum('aux,auf->axf', decayed_key_rows, value_block_rows, precision=HIGH_ACCURACY)
    return (state_matrix, result)

def reference(residual_signal, reading_probe_preactivations, keep_switch_preactivations, written_entries, emission_switch_preactivations, additional_shrink_amount, complement_of_floor, per_group_rescaler, emission_linear_map, channel_layer_rescaler, expanding_linear_map, contracting_linear_map):
    count = TOKENS // BLOCK
    query_act = jax.nn.silu(reading_probe_preactivations.astype(jnp.float32))
    logarithmic_keep_fraction = jnp.logaddexp(jnp.log1p(-complement_of_floor), jnp.log(complement_of_floor) + jax.nn.log_sigmoid(keep_switch_preactivations.astype(jnp.float32))) + additional_shrink_amount
    key_part = -jnp.expm1(logarithmic_keep_fraction)
    value_part = written_entries.astype(jnp.float32)

    def to_blocks(values):
        return values.reshape(count, BLOCK, HEADS, HEAD).transpose(0, 2, 1, 3)
    start = jnp.zeros((HEADS, HEAD, HEAD), jnp.float32)
    ignored, outputs = lax.scan(block_step, start, (to_blocks(query_act), to_blocks(key_part), to_blocks(logarithmic_keep_fraction), to_blocks(value_part)))
    recurrent_output = outputs.transpose(0, 2, 1, 3).reshape(TOKENS, HEADS, HEAD)
    scaled = recurrent_output * lax.rsqrt(lax.optimization_barrier(jnp.mean(recurrent_output * recurrent_output, axis=-1, keepdims=True)) + norm_eps) * per_group_rescaler
    gated = scaled * jax.nn.silu(emission_switch_preactivations.astype(jnp.float32)).reshape(TOKENS, HEADS, HEAD)
    mixed_heads = gated.reshape(TOKENS, MIX).astype(jnp.bfloat16)
    after_mix = residual_signal.astype(jnp.float32) + jnp.dot(mixed_heads, emission_linear_map, preferred_element_type=jnp.float32)
    normed = (after_mix * lax.rsqrt(lax.optimization_barrier(jnp.mean(after_mix * after_mix, axis=-1, keepdims=True)) + norm_eps) * channel_layer_rescaler).astype(jnp.bfloat16)
    upward = jnp.dot(normed, expanding_linear_map, preferred_element_type=jnp.float32)
    hidden = jnp.square(jax.nn.relu(upward)).astype(jnp.bfloat16)
    downward = lax.dot_general(hidden, contracting_linear_map, (((1,), (1,)), ((), ())), preferred_element_type=jnp.float32)
    return (after_mix + downward).astype(jnp.bfloat16)
```

```python
import jax
import jax.numpy as jnp
from jax import lax
from jax.experimental import pallas as pl
from jax.experimental.pallas import tpu as pltpu
from jax.sharding import Mesh
from jax.sharding import PartitionSpec as P

Z, Y, X, C = 16, 4, 4, 2
HEAD = 128
BLOCK = 64
ROWS = 256
D = 2048
MIX = 1024
HID = 1024
NA = 384
NB = HID - NA
SP_N = Z * Y
WR = D // SP_N
STEPS = Z // 2
HALVES = 2
HW = D // HALVES
F32 = jnp.float32
BF16 = jnp.bfloat16
EPS = 1e-06
EXACT = lax.Precision.HIGHEST
NT = (((1,), (1,)), ((), ()))
TN = (((0,), (0,)), ((), ()))


def sigmoid(x):
    return 1.0 / (1.0 + jnp.exp(-x))


def log_one_minus(u):
    series = jnp.zeros_like(u)
    for k in range(9, 0, -1):
        series = u * (1.0 / k + series)
    return jnp.where(u < 0.125, -series, jnp.log(1.0 - u))


def one_minus_exp(w):
    series = jnp.ones_like(w)
    for k in range(10, 1, -1):
        series = 1.0 + (w * (1.0 / k)) * series
    return jnp.where(w > -0.5, -w * series, 1.0 - jnp.exp(w))


def kernel(
    resid,
    read_pre,
    keep_pre,
    written,
    emit_pre,
    shrink,
    floor_c,
    head_gain,
    wout_in,
    norm_gain,
    up_in,
    down_in,
    out,
    wa,
    wb,
    wo,
    after,
    after_scale,
    normed,
    hid_a,
    hid_b,
    heads,
    local_out,
    q_decay,
    mixed,
    ybuf,
    zsend,
    zbuf,
    pbuf,
    pair_out,
    pair_in,
    own_sum,
    rs_out,
    rs_in,
    fin,
    lsem,
    a1_s,
    a1_r,
    a2_s,
    a2_r,
    b1_s,
    b1_r,
    yf_s,
    yf_r,
    yh_s,
    yh_r,
    st_s,
    st_r,
    zs_s,
    zs_r,
    pq_s,
    pq_r,
    wx_s,
    wx_r,
    wc_s,
    wc_r,
    hx_s,
    hx_r,
    hc_s,
    hc_r,
    pp_s,
    pp_r,
    rs_s,
    rs_r,
    gx_s,
    gx_r,
    gc_s,
    gc_r,
):
    z = lax.axis_index("z")
    y = lax.axis_index("y")
    x = lax.axis_index("x")
    c = lax.axis_index("c")
    tp = x * C + c

    def zi(d):
        return lax.rem(z + (d + Z), Z)

    def yi(d):
        return lax.rem(y + (d + Y), Y)

    def xi(d):
        return lax.rem(x + (d + X), X)

    def dev(**kw):
        at = {"z": z, "y": y, "x": x, "c": c}
        at.update(kw)
        return (at["z"], at["y"], at["x"], at["c"])

    def rdma(src, dst, s, r, to):
        return pltpu.make_async_remote_copy(
            src_ref=src,
            dst_ref=dst,
            send_sem=s,
            recv_sem=r,
            device_id=to,
            device_id_type=pl.DeviceIdType.MESH,
        )

    sent = []

    def send(src, dst, s, r, to):
        cp = rdma(src, dst, s, r, to)
        cp.start()
        sent.append(cp)

    def arrive(ref, s, r):
        rdma(ref, ref, s, r, dev(c=1 - c)).wait_recv()

    bar = pltpu.get_barrier_semaphore()
    peers = [dev(z=zi(d)) for d in range(1, Z)]
    peers += [dev(y=yi(d)) for d in range(1, Y)]
    peers += [dev(x=xi(d)) for d in range(1, X)]
    peers += [dev(c=1 - c)]
    for p in peers:
        pl.semaphore_signal(bar, inc=1, device_id=p, device_id_type=pl.DeviceIdType.MESH)

    def rows32(zk, yk, n=WR, off=0):
        return pl.ds(pl.multiple_of((zk * Y + yk) * WR + off, 16), n)

    def a_own():
        return rows32(z, y)

    local = []
    for u, src in ((0, up_in), (1, down_in)):
        local.append(
            pltpu.make_async_copy(src.at[:, pl.ds(0, NA)], wa.at[u, a_own()], lsem.at[2 * u])
        )
        local.append(
            pltpu.make_async_copy(src.at[:, pl.ds(NA, NB)], wb.at[u, a_own()], lsem.at[2 * u + 1])
        )

    def orows(xk, ck, n=HEAD, off=0):
        return pl.ds(pl.multiple_of((xk * C + ck) * HEAD + off, 64), n)

    local.append(pltpu.make_async_copy(wout_in, wo.at[orows(x, c)], lsem.at[4]))
    for cp in local:
        cp.start()

    floor = floor_c[...]
    pre = keep_pre[...].astype(F32)
    logs = log_one_minus(floor * (1.0 / (1.0 + jnp.exp(pre)))) + shrink[...]
    key = one_minus_exp(logs)
    rp = read_pre[...].astype(F32)
    query = rp * sigmoid(rp)
    value = written[...].astype(F32)
    ti = lax.broadcasted_iota(jnp.int32, (BLOCK, BLOCK), 0)
    si = lax.broadcasted_iota(jnp.int32, (BLOCK, BLOCK), 1)
    lower = ti >= si
    tri = lower.astype(F32)
    state = jnp.zeros((HEAD, HEAD), F32)
    base = jnp.zeros((1, HEAD), F32)
    parts = []
    for k in range(ROWS // BLOCK):
        sl = slice(k * BLOCK, (k + 1) * BLOCK)
        lc = jnp.dot(tri, logs[sl], precision=EXACT, preferred_element_type=F32)
        end = lc[BLOCK - 1 :, :]
        kd = key[sl] * jnp.exp(end - lc)
        parts.append((sl, lc, state))
        q_decay[sl, :] = query[sl] * jnp.exp(lc + base)
        state = jnp.exp(end) * state + lax.dot_general(
            value[sl], kd, TN, precision=EXACT, preferred_element_type=F32
        )
        base = base + end
    decay = jnp.exp(base)

    def two_parts(a):
        hi = a.astype(BF16)
        lo = (a - hi.astype(F32)).astype(BF16)
        r = lax.broadcasted_iota(jnp.int32, (16, HEAD), 0)
        both = jnp.where(r == 0, hi.astype(F32), jnp.where(r == 1, lo.astype(F32), 0.0))
        return both.astype(BF16)

    ybuf[y, 0:HEAD, :] = state.astype(BF16)
    ybuf[y, HEAD : HEAD + 16, :] = two_parts(decay)

    for cp in local:
        cp.wait()
    pl.semaphore_wait(bar, len(peers))

    for d in range(1, Y):
        send(ybuf.at[y], ybuf.at[y], st_s.at[d], st_r.at[d], dev(y=yi(d)))
    for u in range(2):
        for d in range(1, Y):
            ref = wa.at[u, a_own()]
            send(ref, ref, a1_s.at[u, d], a1_r.at[u, d], dev(y=yi(d)))

    def send_b(i, step, zk):
        for u in range(2):
            ref = wb.at[u, rows32(zk, y)]
            send(ref, ref, b1_s.at[i, u, step], b1_r.at[i, u, step], dev(z=zi(1 - 2 * i)))

    def send_y(k, zk):
        for u in range(2):
            ref = wb.at[u, rows32(zk, y)]
            for i in range(2):
                send(ref, ref, yf_s.at[i, u, k], yf_r.at[i, u, k], dev(y=yi(1 - 2 * i)))

    def relay_y(k, zk):
        for u in range(2):
            for i in range(2):
                yk = yi(2 * i - 1)
                arrive(wb.at[u, rows32(zk, yk)], yf_s.at[i, u, k], yf_r.at[i, u, k])
                ref = wb.at[u, rows32(zk, yk, 16, 16 * i)]
                send(ref, ref, yh_s.at[i, u, k], yh_r.at[i, u, k], dev(y=yi(1 - 2 * i)))

    def end_y(k, zk):
        for u in range(2):
            for i in range(2):
                ref = wb.at[u, rows32(zk, yi(2), 16, 16 * i)]
                arrive(ref, yh_s.at[i, u, k], yh_r.at[i, u, k])

    def group(zk):
        return pl.ds(pl.multiple_of(zk * (Y * WR), Y * WR), Y * WR)

    def send_a(i, step, zk):
        for u in range(2):
            ref = wa.at[u, group(zk)]
            send(ref, ref, a2_s.at[i, u, step], a2_r.at[i, u, step], dev(z=zi(1 - 2 * i)))

    for i in range(2):
        send_b(i, 1, z)
    own_wo = wo.at[orows(x, c)]
    for i in range(2):
        send(own_wo, own_wo, wx_s.at[i], wx_r.at[i], dev(x=xi(1 - 2 * i)))
    send(own_wo, own_wo, wc_s.at[0], wc_r.at[0], dev(c=1 - c))
    send_y(0, z)

    for sl, lc, st in parts:
        qd = query[sl] * jnp.exp(lc)
        kd = key[sl] * jnp.exp(-lc)
        scores = lax.dot_general(qd, kd, NT, precision=EXACT, preferred_element_type=F32)
        scores = jnp.where(lower, scores, 0.0)
        local_out[sl, :] = jnp.dot(
            scores, value[sl], precision=EXACT, preferred_element_type=F32
        ) + lax.dot_general(qd, st, NT, precision=EXACT, preferred_element_type=F32)

    for u in range(2):
        for d in range(1, Y):
            arrive(wa.at[u, rows32(z, yi(-d))], a1_s.at[u, d], a1_r.at[u, d])
    for i in range(2):
        send_a(i, 1, z)

    def decay_of(block):
        return block[0:1, :].astype(F32) + block[1:2, :].astype(F32)

    for d in range(1, Y):
        arrive(ybuf.at[yi(-d)], st_s.at[d], st_r.at[d])
    quarter = pl.ds(pl.multiple_of(y * (HEAD // Y), HEAD // Y), HEAD // Y)
    row_q = jnp.zeros((HEAD // Y, HEAD), F32)
    row_a = jnp.ones((1, HEAD), F32)
    for k in range(Y):
        a_k = decay_of(ybuf[k, HEAD : HEAD + 16, :])
        row_q = a_k * row_q + ybuf[k, quarter, :].astype(F32)
        row_a = row_a * a_k
    zsend[0 : HEAD // Y, :] = row_q.astype(BF16)
    zsend[HEAD // Y : HEAD // Y + 16, :] = two_parts(row_a)
    for d in range(1, Z):

        @pl.when(z + d < Z)
        def _():
            rdma(zsend, zbuf.at[z], zs_s.at[d], zs_r.at[d], dev(z=zi(d))).start()

    def stage_wout():
        for i in range(2):
            xk = xi(2 * i - 1)
            full = wo.at[orows(xk, c)]
            arrive(full, wx_s.at[i], wx_r.at[i])
            half = wo.at[orows(xk, c, 64, 64 * i)]
            send(half, half, wx_s.at[2 + i], wx_r.at[2 + i], dev(x=xi(1 - 2 * i)))
            send(full, full, wc_s.at[1 + i], wc_r.at[1 + i], dev(c=1 - c))

    def stage_wout2():
        for i in range(2):
            half = wo.at[orows(xi(2), c, 64, 64 * i)]
            arrive(half, wx_s.at[2 + i], wx_r.at[2 + i])
            send(half, half, wc_s.at[3 + i], wc_r.at[3 + i], dev(c=1 - c))

    def stage_z():
        for d in range(1, Z):

            @pl.when(z - d >= 0)
            def _():
                arrive(zbuf.at[zi(-d)], zs_s.at[d], zs_r.at[d])

        def add(k, acc):
            a_k = decay_of(zbuf[k, HEAD // Y : HEAD // Y + 16, :])
            return a_k * acc + zbuf[k, 0 : HEAD // Y, :].astype(F32)

        pbuf[quarter, :] = lax.fori_loop(0, z, add, jnp.zeros((HEAD // Y, HEAD), F32))
        for d in range(1, Y):
            ref = pbuf.at[quarter]
            send(ref, ref, pq_s.at[d], pq_r.at[d], dev(y=yi(d)))

    def stage_heads():
        for d in range(1, Y):
            there = pl.ds(pl.multiple_of(yi(-d) * (HEAD // Y), HEAD // Y), HEAD // Y)
            arrive(pbuf.at[there], pq_s.at[d], pq_r.at[d])
        prior = pbuf[...]
        for k in range(Y - 1):
            a_k = decay_of(ybuf[k, HEAD : HEAD + 16, :])
            prior = jnp.where(k < y, a_k * prior + ybuf[k, 0:HEAD, :].astype(F32), prior)
        recur = local_out[...] + lax.dot_general(
            q_decay[...], prior, NT, precision=EXACT, preferred_element_type=F32
        )
        ep = emit_pre[...].astype(F32)
        norm = lax.rsqrt(jnp.mean(recur * recur, axis=-1, keepdims=True) + EPS)
        mixed[...] = (recur * norm * head_gain[...] * (ep * sigmoid(ep))).astype(BF16)
        heads[:, cols(x, c)] = mixed[...]
        dst = heads.at[:, cols(x, c)]
        for d in range(1, X):
            send(mixed, dst, hx_s.at[d], hx_r.at[d], dev(x=xi(d)))
        send(mixed, dst, hc_s.at[0], hc_r.at[0], dev(c=1 - c))

    def cols(xk, ck):
        return pl.ds(pl.multiple_of((xk * C + ck) * HEAD, HEAD), HEAD)

    def stage_heads2():
        for d in range(1, X):
            ref = heads.at[:, cols(xi(-d), c)]
            arrive(ref, hx_s.at[d], hx_r.at[d])
            send(ref, ref, hc_s.at[d], hc_r.at[d], dev(c=1 - c))

    def stage_norm():
        for i in range(2):
            arrive(wo.at[orows(xi(2 * i - 1), 1 - c)], wc_s.at[1 + i], wc_r.at[1 + i])
            arrive(wo.at[orows(xi(2), 1 - c, 64, 64 * i)], wc_s.at[3 + i], wc_r.at[3 + i])
        arrive(wo.at[orows(x, 1 - c)], wc_s.at[0], wc_r.at[0])
        for d in range(0, X):
            arrive(heads.at[:, cols(xi(-d), 1 - c)], hc_s.at[d], hc_r.at[d])
        tile = 256

        def project(n, square):
            at = pl.ds(pl.multiple_of(n * tile, tile), tile)
            got = resid[:, at].astype(F32) + jnp.dot(
                heads[...], wo[:, at], preferred_element_type=F32
            )
            after[:, at] = got
            return square + jnp.sum(got * got, axis=-1, keepdims=True)

        square = lax.fori_loop(0, D // tile, project, jnp.zeros((ROWS, 1), F32))
        after_scale[...] = lax.rsqrt(square * (1.0 / D) + EPS)

        def scaled(n, carry):
            at = pl.ds(pl.multiple_of(n * tile, tile), tile)
            for j in range(2):
                half = pl.ds(pl.multiple_of(jnp.where(j == 0, 1 - c, c) * 128, 128), 128)
                normed[128 * j : 128 * (j + 1), at] = (
                    after[half, at] * after_scale[half, :] * norm_gain[:, at]
                ).astype(BF16)
            return carry

        lax.fori_loop(0, D // tile, scaled, 0)

    stages = {
        1: [stage_wout],
        2: [stage_z],
        3: [stage_heads, stage_wout2],
        4: [stage_heads2],
        5: [stage_norm],
    }

    pending = [(0, z)]
    ended = []
    for step in range(1, STEPS + 1):
        fresh = []
        for i in range(2):
            if i == 1 and step == STEPS:
                continue
            zk = zi((2 * i - 1) * step)
            for u in range(2):
                arrive(wb.at[u, rows32(zk, y)], b1_s.at[i, u, step], b1_r.at[i, u, step])
            if step + 1 <= STEPS - i:
                send_b(i, step + 1, zk)
            k = 2 * step - 1 + i
            send_y(k, zk)
            fresh.append((k, zk))
        for i in range(2):
            if i == 1 and step == STEPS:
                continue
            zk = zi((2 * i - 1) * step)
            for u in range(2):
                arrive(wa.at[u, group(zk)], a2_s.at[i, u, step], a2_r.at[i, u, step])
                if step + 1 <= STEPS - i:
                    ref = wa.at[u, group(zk)]
                    send(
                        ref,
                        ref,
                        a2_s.at[i, u, step + 1],
                        a2_r.at[i, u, step + 1],
                        dev(z=zi(1 - 2 * i)),
                    )
        for k, zk in pending:
            relay_y(k, zk)
        for k, zk in ended:
            end_y(k, zk)
        ended, pending = pending, fresh
        for stage in stages.get(step, []):
            stage()
    for k, zk in pending:
        relay_y(k, zk)
    for k, zk in ended + pending:
        end_y(k, zk)

    for buf, w, width in ((hid_a, wa, NA), (hid_b, wb, NB)):
        for at in range(0, width, 256):
            n = min(256, width - at)
            h = jnp.dot(normed[...], w[0, :, at : at + n], preferred_element_type=F32)
            h = jnp.maximum(h, 0.0)
            buf[:, at : at + n] = (h * h).astype(BF16)
    tile = 256
    per = HW // tile
    for h in range(HALVES):

        def contract(n, carry, h=h):
            fr = pl.ds(pl.multiple_of(h * HW + n * tile, tile), tile)
            at = pl.ds(pl.multiple_of(n * tile, tile), tile)
            got = lax.dot_general(hid_a[...], wa[1, fr, :], NT, preferred_element_type=F32)
            got += lax.dot_general(hid_b[...], wb[1, fr, :], NT, preferred_element_type=F32)
            pair_out[h, :, at] = got[0:128].astype(BF16)
            own_sum[h, :, at] = got[128:256]
            return carry

        lax.fori_loop(0, per, contract, 0)
        send(pair_out.at[h], pair_in.at[h], pp_s.at[h], pp_r.at[h], dev(c=1 - c))

    def blk(xk):
        return pl.ds(pl.multiple_of(xk * 32, 32), 32)

    for h in range(HALVES):
        arrive(pair_in.at[h], pp_s.at[h], pp_r.at[h])
        own_sum[h] = own_sum[h] + pair_in[h].astype(F32)
        for d in range(1, X):
            rs_out[h, d - 1] = own_sum[h, blk(xi(d)), :].astype(BF16)
            send(
                rs_out.at[h, d - 1],
                rs_in.at[h, d - 1],
                rs_s.at[h, d],
                rs_r.at[h, d],
                dev(x=xi(d)),
            )

    def orow(xk, ck):
        return pl.ds(pl.multiple_of(ck * 128 + xk * 32, 32), 32)

    for h in range(HALVES):
        hc = pl.ds(h * HW, HW)
        total = after[orow(x, c), hc] + own_sum[h, blk(x), :]
        for d in range(1, X):
            arrive(rs_in.at[h, d - 1], rs_s.at[h, d], rs_r.at[h, d])
            total = total + rs_in[h, d - 1].astype(F32)
        fin[h] = total.astype(BF16)
        out[orow(x, c), hc] = fin[h]
        dst = out.at[orow(x, c), hc]
        for d in range(1, X):
            send(fin.at[h], dst, gx_s.at[h, d], gx_r.at[h, d], dev(x=xi(d)))
        send(fin.at[h], dst, gc_s.at[h, 0], gc_r.at[h, 0], dev(c=1 - c))
    for h in range(HALVES):
        hc = pl.ds(h * HW, HW)
        for d in range(1, X):
            ref = out.at[orow(xi(-d), c), hc]
            arrive(ref, gx_s.at[h, d], gx_r.at[h, d])
            send(ref, ref, gc_s.at[h, d], gc_r.at[h, d], dev(c=1 - c))
    for h in range(HALVES):
        hc = pl.ds(h * HW, HW)
        for d in range(0, X):
            arrive(out.at[orow(xi(-d), 1 - c), hc], gc_s.at[h, d], gc_r.at[h, d])
    for cp in sent:
        cp.wait_send()
    for d in range(1, Z):

        @pl.when(z + d < Z)
        def _():
            rdma(zsend, zbuf.at[z], zs_s.at[d], zs_r.at[d], dev(z=zi(d))).wait_send()


def body(
    resid,
    read_pre,
    keep_pre,
    written,
    emit_pre,
    shrink,
    floor_c,
    head_gain,
    wout,
    norm_gain,
    up,
    down,
):
    vm = pl.BlockSpec(memory_space=pltpu.VMEM)
    hbm = pl.BlockSpec(memory_space=pltpu.HBM)
    dma = pltpu.SemaphoreType.DMA
    call = pl.pallas_call(
        kernel,
        out_shape=jax.ShapeDtypeStruct((ROWS, D), BF16),
        in_specs=[vm] * 8 + [hbm, vm, hbm, hbm],
        out_specs=vm,
        scratch_shapes=[
            pltpu.VMEM((2, D, NA), BF16),
            pltpu.VMEM((2, D, NB), BF16),
            pltpu.VMEM((MIX, D), BF16),
            pltpu.VMEM((ROWS, D), F32),
            pltpu.VMEM((ROWS, 1), F32),
            pltpu.VMEM((ROWS, D), BF16),
            pltpu.VMEM((ROWS, NA), BF16),
            pltpu.VMEM((ROWS, NB), BF16),
            pltpu.VMEM((ROWS, MIX), BF16),
            pltpu.VMEM((ROWS, HEAD), F32),
            pltpu.VMEM((ROWS, HEAD), F32),
            pltpu.VMEM((ROWS, HEAD), BF16),
            pltpu.VMEM((Y, HEAD + 16, HEAD), BF16),
            pltpu.VMEM((HEAD // Y + 16, HEAD), BF16),
            pltpu.VMEM((Z, HEAD // Y + 16, HEAD), BF16),
            pltpu.VMEM((HEAD, HEAD), F32),
            pltpu.VMEM((HALVES, 128, HW), BF16),
            pltpu.VMEM((HALVES, 128, HW), BF16),
            pltpu.VMEM((HALVES, 128, HW), F32),
            pltpu.VMEM((HALVES, X - 1, 32, HW), BF16),
            pltpu.VMEM((HALVES, X - 1, 32, HW), BF16),
            pltpu.VMEM((HALVES, 32, HW), BF16),
            dma((5,)),
            dma((2, Y)),
            dma((2, Y)),
            dma((2, 2, STEPS + 1)),
            dma((2, 2, STEPS + 1)),
            dma((2, 2, STEPS + 1)),
            dma((2, 2, STEPS + 1)),
            dma((2, 2, Z)),
            dma((2, 2, Z)),
            dma((2, 2, Z)),
            dma((2, 2, Z)),
            dma((Y,)),
            dma((Y,)),
            dma((Z,)),
            dma((Z,)),
            dma((Y,)),
            dma((Y,)),
            dma((4,)),
            dma((4,)),
            dma((5,)),
            dma((5,)),
            dma((X,)),
            dma((X,)),
            dma((X,)),
            dma((X,)),
            dma((HALVES,)),
            dma((HALVES,)),
            dma((HALVES, X)),
            dma((HALVES, X)),
            dma((HALVES, X)),
            dma((HALVES, X)),
            dma((HALVES, X)),
            dma((HALVES, X)),
        ],
        compiler_params=pltpu.CompilerParams(
            collective_id=0, has_side_effects=True, vmem_limit_bytes=60 * 1024 * 1024
        ),
        name="layer",
    )
    return call(
        resid,
        read_pre,
        keep_pre,
        written,
        emit_pre,
        shrink,
        floor_c.reshape(1, -1),
        head_gain.reshape(1, -1),
        wout,
        norm_gain.reshape(1, -1),
        up,
        down,
    )


def solution(mesh):
    finer = Mesh(mesh.devices.reshape(Z, Y, X, C), ("z", "y", "x", "c"))
    sp, tp = ("z", "y"), ("x", "c")
    return jax.shard_map(
        body,
        mesh=finer,
        in_specs=(
            P(sp, None),
            P(sp, tp),
            P(sp, tp),
            P(sp, tp),
            P(sp, tp),
            P(sp, tp),
            P(tp),
            P(),
            P(tp, None),
            P(),
            P(sp, tp),
            P(sp, tp),
        ),
        out_specs=P(sp, None),
        check_vma=False,
    )
```

```python
import jax
import jax.numpy as jnp
from jax import lax
from jax.experimental import pallas as pl
from jax.experimental.pallas import tpu as pltpu
from jax.sharding import Mesh
from jax.sharding import PartitionSpec as P

Z, Y, X, C = 16, 4, 4, 2
HEAD = 128
BLOCK = 64
ROWS = 256
D = 2048
MIX = 1024
HID = 1024
NA = 384
NB = HID - NA
SP_N = Z * Y
WR = D // SP_N
G = 4
STEPS = Z // 2
LAG = 0
CUTS = ((10, 4), (12, 10), (13, 16))
NB_CUT = len(CUTS)
F32 = jnp.float32
BF16 = jnp.bfloat16
EPS = 1e-06
EXACT = lax.Precision.HIGHEST
NT = (((1,), (1,)), ((), ()))
TN = (((0,), (0,)), ((), ()))


def sigmoid(x):
    return 1.0 / (1.0 + jnp.exp(-x))


def log_one_minus(u):
    series = jnp.zeros_like(u)
    for k in range(9, 0, -1):
        series = u * (1.0 / k + series)
    return jnp.where(u < 0.125, -series, jnp.log(1.0 - u))


def one_minus_exp(w):
    series = jnp.ones_like(w)
    for k in range(10, 1, -1):
        series = 1.0 + (w * (1.0 / k)) * series
    return jnp.where(w > -0.5, -w * series, 1.0 - jnp.exp(w))


def kernel(
    resid_in,
    read_in,
    keep_in,
    written_in,
    emit_in,
    shrink_in,
    floor_in,
    head_gain_in,
    wout_in,
    norm_gain_in,
    up_in,
    down_in,
    out,
    wa,
    wb,
    wo,
    read_pre,
    keep_pre,
    written,
    emit_pre,
    shrink,
    floor_c,
    head_gain,
    norm_gain,
    resid,
    after,
    after_scale,
    normed,
    hid_a,
    hid_b,
    heads,
    local_out,
    q_decay,
    mixed,
    ybuf,
    zsend,
    zbuf,
    gsend,
    gbuf,
    pbuf,
    pair_out,
    pair_in,
    own_sum,
    rs_out,
    rs_in,
    ag,
    know,
    lsem,
    a1_s,
    a1_r,
    a2_s,
    a2_r,
    b1_s,
    b1_r,
    yf_s,
    yf_r,
    yh_s,
    yh_r,
    st_s,
    st_r,
    zs_s,
    zs_r,
    gs_s,
    gs_r,
    pq_s,
    pq_r,
    wx_s,
    wx_r,
    wc_s,
    wc_r,
    hx_s,
    hx_r,
    hc_s,
    hc_r,
    pp_s,
    pp_r,
    rs_s,
    rs_r,
    gx_s,
    gx_r,
    gc_s,
    gc_r,
):
    z = lax.axis_index("z")
    y = lax.axis_index("y")
    x = lax.axis_index("x")
    c = lax.axis_index("c")
    tp = x * C + c

    def zi(d):
        return lax.rem(z + (d + Z), Z)

    def yi(d):
        return lax.rem(y + (d + Y), Y)

    def xi(d):
        return lax.rem(x + (d + X), X)

    def dev(**kw):
        at = {"z": z, "y": y, "x": x, "c": c}
        at.update(kw)
        return (at["z"], at["y"], at["x"], at["c"])

    def rdma(src, dst, s, r, to):
        return pltpu.make_async_remote_copy(
            src_ref=src,
            dst_ref=dst,
            send_sem=s,
            recv_sem=r,
            device_id=to,
            device_id_type=pl.DeviceIdType.MESH,
        )

    sent = []

    def send(src, dst, s, r, to):
        cp = rdma(src, dst, s, r, to)
        cp.start()
        sent.append(cp)

    def arrive(ref, s, r):
        rdma(ref, ref, s, r, dev(c=1 - c)).wait_recv()

    bar = pltpu.get_barrier_semaphore()
    peers = [dev(z=zi(d)) for d in (1, Z - 1)]
    peers += [dev(y=yi(d)) for d in range(1, Y)]
    peers += [dev(x=xi(d)) for d in range(1, X)]
    peers += [dev(c=1 - c)]
    for p in peers:
        pl.semaphore_signal(bar, inc=1, device_id=p, device_id_type=pl.DeviceIdType.MESH)

    def rows32(zk, yk, n=WR, off=0):
        return pl.ds(pl.multiple_of((zk * Y + yk) * WR + off, 16), n)

    def a_own():
        return rows32(z, y)

    local = []
    for u, src in ((0, up_in), (1, down_in)):
        local.append(
            pltpu.make_async_copy(src.at[:, pl.ds(0, NA)], wa.at[u, a_own()], lsem.at[2 * u])
        )
        local.append(
            pltpu.make_async_copy(src.at[:, pl.ds(NA, NB)], wb.at[u, a_own()], lsem.at[2 * u + 1])
        )

    def orows(xk, ck, n=HEAD, off=0):
        return pl.ds(pl.multiple_of((xk * C + ck) * HEAD + off, 64), n)

    local.append(pltpu.make_async_copy(wout_in, wo.at[orows(x, c)], lsem.at[4]))
    for cp in local:
        cp.start()
    small = []
    for src, dst in (
        (floor_in, floor_c),
        (keep_in, keep_pre),
        (shrink_in, shrink),
        (read_in, read_pre),
        (written_in, written),
        (emit_in, emit_pre),
        (head_gain_in, head_gain),
        (norm_gain_in, norm_gain),
    ):
        small.append(pltpu.make_async_copy(src, dst, lsem.at[6 + len(small)]))
    for cp in small:
        cp.start()
    resid_copy = pltpu.make_async_copy(resid_in, resid, lsem.at[5])
    resid_copy.start()

    for cp in local:
        cp.wait()
    pl.semaphore_wait(bar, len(peers))

    def tell(n):
        for d in (1 << n, Z - (1 << n)):
            pl.semaphore_signal(
                know.at[n], inc=1, device_id=dev(z=zi(d)), device_id_type=pl.DeviceIdType.MESH
            )

    tell(0)
    def send_b(u, i, step, zk):
        ref = wb.at[u, rows32(zk, y)]
        send(ref, ref, b1_s.at[i, u, step], b1_r.at[i, u, step], dev(z=zi(1 - 2 * i)))

    def send_y(u, k, zk):
        ref = wb.at[u, rows32(zk, y)]
        for i in range(2):
            send(ref, ref, yf_s.at[i, u, k], yf_r.at[i, u, k], dev(y=yi(1 - 2 * i)))

    def relay_y(u, k, zk):
        for i in range(2):
            yk = yi(2 * i - 1)
            arrive(wb.at[u, rows32(zk, yk)], yf_s.at[i, u, k], yf_r.at[i, u, k])
            ref = wb.at[u, rows32(zk, yk, 16, 16 * i)]
            send(ref, ref, yh_s.at[i, u, k], yh_r.at[i, u, k], dev(y=yi(1 - 2 * i)))

    def end_y(u, k, zk):
        for i in range(2):
            ref = wb.at[u, rows32(zk, yi(2), 16, 16 * i)]
            arrive(ref, yh_s.at[i, u, k], yh_r.at[i, u, k])

    def group(zk):
        return pl.ds(pl.multiple_of(zk * (Y * WR), Y * WR), Y * WR)

    def send_a(u, i, step, zk, j):
        ref = wa.at[u, group(zk)]
        send(ref, ref, a2_s.at[i, u, step, j], a2_r.at[i, u, step, j], dev(z=zi(1 - 2 * i)))

    for i in range(2):
        send_b(0, i, 1, z)
    for u in range(2):
        for d in range(1, Y):
            ref = wa.at[u, a_own()]
            send(ref, ref, a1_s.at[u, d], a1_r.at[u, d], dev(y=yi(d)))
    for u in range(2):
        send_y(u, 0, z)
    own_wo = wo.at[orows(x, c)]
    for i in range(2):
        send(own_wo, own_wo, wx_s.at[i], wx_r.at[i], dev(x=xi(1 - 2 * i)))
    send(own_wo, own_wo, wc_s.at[0], wc_r.at[0], dev(c=1 - c))

    for cp in small:
        cp.wait()
    floor = floor_c[...]
    pre = keep_pre[...].astype(F32)
    logs = log_one_minus(floor * (1.0 / (1.0 + jnp.exp(pre)))) + shrink[...]
    key = one_minus_exp(logs)
    rp = read_pre[...].astype(F32)
    query = rp * sigmoid(rp)
    value = written[...].astype(F32)
    ti = lax.broadcasted_iota(jnp.int32, (BLOCK, BLOCK), 0)
    si = lax.broadcasted_iota(jnp.int32, (BLOCK, BLOCK), 1)
    lower = ti >= si
    tri = lower.astype(F32)
    state = jnp.zeros((HEAD, HEAD), F32)
    base = jnp.zeros((1, HEAD), F32)
    parts = []
    for k in range(ROWS // BLOCK):
        sl = slice(k * BLOCK, (k + 1) * BLOCK)
        lc = jnp.dot(tri, logs[sl], precision=EXACT, preferred_element_type=F32)
        end = lc[BLOCK - 1 :, :]
        kd = key[sl] * jnp.exp(end - lc)
        parts.append((sl, lc, state))
        q_decay[sl, :] = query[sl] * jnp.exp(lc + base)
        state = jnp.exp(end) * state + lax.dot_general(
            value[sl], kd, TN, precision=EXACT, preferred_element_type=F32
        )
        base = base + end
    decay = jnp.exp(base)

    def two_parts(a):
        hi = a.astype(BF16)
        lo = (a - hi.astype(F32)).astype(BF16)
        r = lax.broadcasted_iota(jnp.int32, (16, HEAD), 0)
        both = jnp.where(r == 0, hi.astype(F32), jnp.where(r == 1, lo.astype(F32), 0.0))
        return both.astype(BF16)

    ybuf[y, 0:HEAD, :] = state.astype(BF16)
    ybuf[y, HEAD : HEAD + 16, :] = two_parts(decay)

    for d in range(1, Y):
        send(ybuf.at[y], ybuf.at[y], st_s.at[d], st_r.at[d], dev(y=yi(d)))

    for sl, lc, st in parts:
        qd = query[sl] * jnp.exp(lc)
        kd = key[sl] * jnp.exp(-lc)
        scores = lax.dot_general(qd, kd, NT, precision=EXACT, preferred_element_type=F32)
        scores = jnp.where(lower, scores, 0.0)
        local_out[sl, :] = jnp.dot(
            scores, value[sl], precision=EXACT, preferred_element_type=F32
        ) + lax.dot_general(qd, st, NT, precision=EXACT, preferred_element_type=F32)

    pl.semaphore_wait(know.at[0], 2)
    tell(1)
    for u in range(2):
        for d in range(1, Y):
            arrive(wa.at[u, rows32(z, yi(-d))], a1_s.at[u, d], a1_r.at[u, d])
        if u == 0:
            for i in range(2):
                send_a(0, i, 1, z, 0)
    for i in range(2):
        send_b(1, i, 1, z)
    for i in range(2):
        send_a(1, i, 1, z, 0)

    def decay_of(block):
        return block[0:1, :].astype(F32) + block[1:2, :].astype(F32)

    for d in range(1, Y):
        arrive(ybuf.at[yi(-d)], st_s.at[d], st_r.at[d])
    quarter = pl.ds(pl.multiple_of(y * (HEAD // Y), HEAD // Y), HEAD // Y)
    row_q = jnp.zeros((HEAD // Y, HEAD), F32)
    row_a = jnp.ones((1, HEAD), F32)
    for k in range(Y):
        a_k = decay_of(ybuf[k, HEAD : HEAD + 16, :])
        row_q = a_k * row_q + ybuf[k, quarter, :].astype(F32)
        row_a = row_a * a_k
    zsend[0 : HEAD // Y, :] = row_q.astype(BF16)
    zsend[HEAD // Y : HEAD // Y + 16, :] = two_parts(row_a)

    grp = z // G
    inner = z % G

    def zg(d):
        return grp * G + lax.rem(inner + (d + G), G)

    def stage_zsend():
        pl.semaphore_wait(know.at[1], 2)
        tell(2)
        for d in range(1, G):
            send(zsend, zbuf.at[inner], zs_s.at[d], zs_r.at[d], dev(z=zg(d)))

    def decay_rows(ref, k):
        return decay_of(ref[k, HEAD // Y : HEAD // Y + 16, :])

    def stage_zgroup():
        for d in range(1, G):
            arrive(zbuf.at[lax.rem(inner + (G - d), G)], zs_s.at[d], zs_r.at[d])
        zbuf[inner] = zsend[...]
        pl.semaphore_wait(know.at[2], 2)
        total = jnp.zeros((HEAD // Y, HEAD), F32)
        total_a = jnp.ones((1, HEAD), F32)
        for k in range(G):
            a_k = decay_rows(zbuf, k)
            total = a_k * total + zbuf[k, 0 : HEAD // Y, :].astype(F32)
            total_a = total_a * a_k
        gsend[0 : HEAD // Y, :] = total.astype(BF16)
        gsend[HEAD // Y : HEAD // Y + 16, :] = two_parts(total_a)
        for d in range(1, Z // G):

            @pl.when(grp + d < Z // G)
            def _():
                rdma(gsend, gbuf.at[grp], gs_s.at[d], gs_r.at[d], dev(z=zi(d * G))).start()

    def stage_wout():
        for i in range(2):
            xk = xi(2 * i - 1)
            full = wo.at[orows(xk, c)]
            arrive(full, wx_s.at[i], wx_r.at[i])
            half = wo.at[orows(xk, c, 64, 64 * i)]
            send(half, half, wx_s.at[2 + i], wx_r.at[2 + i], dev(x=xi(1 - 2 * i)))
            send(full, full, wc_s.at[1 + i], wc_r.at[1 + i], dev(c=1 - c))

    def stage_wout2():
        for i in range(2):
            half = wo.at[orows(xi(2), c, 64, 64 * i)]
            arrive(half, wx_s.at[2 + i], wx_r.at[2 + i])
            send(half, half, wc_s.at[3 + i], wc_r.at[3 + i], dev(c=1 - c))

    def stage_z():
        for d in range(1, Z // G):

            @pl.when(grp - d >= 0)
            def _():
                arrive(gbuf.at[grp - d], gs_s.at[d], gs_r.at[d])

        def add(k, acc):
            return decay_rows(gbuf, k) * acc + gbuf[k, 0 : HEAD // Y, :].astype(F32)

        def add_in(k, acc):
            return decay_rows(zbuf, k) * acc + zbuf[k, 0 : HEAD // Y, :].astype(F32)

        before = lax.fori_loop(0, grp, add, jnp.zeros((HEAD // Y, HEAD), F32))
        pbuf[quarter, :] = lax.fori_loop(0, inner, add_in, before)
        for d in range(1, Y):
            ref = pbuf.at[quarter]
            send(ref, ref, pq_s.at[d], pq_r.at[d], dev(y=yi(d)))

    def stage_heads():
        for d in range(1, Y):
            there = pl.ds(pl.multiple_of(yi(-d) * (HEAD // Y), HEAD // Y), HEAD // Y)
            arrive(pbuf.at[there], pq_s.at[d], pq_r.at[d])
        prior = pbuf[...]
        for k in range(Y - 1):
            a_k = decay_of(ybuf[k, HEAD : HEAD + 16, :])
            prior = jnp.where(k < y, a_k * prior + ybuf[k, 0:HEAD, :].astype(F32), prior)
        recur = local_out[...] + lax.dot_general(
            q_decay[...], prior, NT, precision=EXACT, preferred_element_type=F32
        )
        ep = emit_pre[...].astype(F32)
        norm = lax.rsqrt(jnp.mean(recur * recur, axis=-1, keepdims=True) + EPS)
        mixed[...] = (recur * norm * head_gain[...] * (ep * sigmoid(ep))).astype(BF16)
        heads[:, cols(x, c)] = mixed[...]
        dst = heads.at[:, cols(x, c)]
        for d in range(1, X):
            send(mixed, dst, hx_s.at[d], hx_r.at[d], dev(x=xi(d)))
        send(mixed, dst, hc_s.at[0], hc_r.at[0], dev(c=1 - c))

    def cols(xk, ck):
        return pl.ds(pl.multiple_of((xk * C + ck) * HEAD, HEAD), HEAD)

    def stage_heads2():
        for d in range(1, X):
            ref = heads.at[:, cols(xi(-d), c)]
            arrive(ref, hx_s.at[d], hx_r.at[d])
            send(ref, ref, hc_s.at[d], hc_r.at[d], dev(c=1 - c))

    tile = 256

    def stage_gathered():
        for i in range(2):
            arrive(wo.at[orows(xi(2 * i - 1), 1 - c)], wc_s.at[1 + i], wc_r.at[1 + i])
            arrive(wo.at[orows(xi(2), 1 - c, 64, 64 * i)], wc_s.at[3 + i], wc_r.at[3 + i])
        arrive(wo.at[orows(x, 1 - c)], wc_s.at[0], wc_r.at[0])
        for d in range(0, X):
            arrive(heads.at[:, cols(xi(-d), 1 - c)], hc_s.at[d], hc_r.at[d])
        resid_copy.wait()
        after_scale[...] = jnp.zeros((ROWS, 1), F32)

    def stage_project(lo, hi):
        def project(n, square):
            at = pl.ds(pl.multiple_of(n * tile, tile), tile)
            got = resid[:, at].astype(F32) + jnp.dot(
                heads[...], wo[:, at], preferred_element_type=F32
            )
            after[:, at] = got
            return square + jnp.sum(got * got, axis=-1, keepdims=True)

        after_scale[...] = lax.fori_loop(lo, hi, project, after_scale[...])

    def stage_norm():
        after_scale[...] = lax.rsqrt(after_scale[...] * (1.0 / D) + EPS)

        def scaled(n, carry):
            at = pl.ds(pl.multiple_of(n * tile, tile), tile)
            for j in range(2):
                half = pl.ds(pl.multiple_of(jnp.where(j == 0, 1 - c, c) * 128, 128), 128)
                normed[128 * j : 128 * (j + 1), at] = (
                    after[half, at] * after_scale[half, :] * norm_gain[:, at]
                ).astype(BF16)
            return carry

        lax.fori_loop(0, D // tile, scaled, 0)

    def stage_up():
        for buf, w, width in ((hid_a, wa, NA), (hid_b, wb, NB)):
            for at in range(0, width, 256):
                n = min(256, width - at)
                h = jnp.dot(normed[...], w[0, :, at : at + n], preferred_element_type=F32)
                h = jnp.maximum(h, 0.0)
                buf[:, at : at + n] = (h * h).astype(BF16)

    def zk_of(k):
        return zi(k // 2 if k % 2 == 0 else -(k + 1) // 2)

    def blk(xk):
        return pl.ds(pl.multiple_of(xk * 32, 32), 32)

    def feat(k):
        return pl.ds(pl.multiple_of(zk_of(k) * 128, 128), 128)

    cuts = [(0 if b == 0 else CUTS[b - 1][1], CUTS[b][1]) for b in range(NB_CUT)]

    def down(b):
        lo, hi = cuts[b]
        for k in range(lo, hi):
            fr = feat(k)
            got = lax.dot_general(hid_a[...], wa[1, fr, :], NT, preferred_element_type=F32)
            got += lax.dot_general(hid_b[...], wb[1, fr, :], NT, preferred_element_type=F32)
            pair_out[k] = got[0:128].astype(BF16)
            own_sum[k] = got[128:256]
        part = pl.ds(lo, hi - lo)
        send(pair_out.at[part], pair_in.at[part], pp_s.at[b], pp_r.at[b], dev(c=1 - c))

    def scatter(b):
        lo, hi = cuts[b]
        part = pl.ds(lo, hi - lo)
        arrive(pair_in.at[part], pp_s.at[b], pp_r.at[b])
        own_sum[lo:hi] = own_sum[lo:hi] + pair_in[lo:hi].astype(F32)
        for d in range(1, X):
            rs_out[d - 1, lo:hi] = own_sum[lo:hi, blk(xi(d)), :].astype(BF16)
            src, dst = rs_out.at[d - 1, part], rs_in.at[d - 1, part]
            send(src, dst, rs_s.at[b, d], rs_r.at[b, d], dev(x=xi(d)))

    own_rows = pl.ds(pl.multiple_of(c * 128 + x * 32, 32), 32)

    def finish(b):
        lo, hi = cuts[b]
        part = pl.ds(lo, hi - lo)
        for d in range(1, X):
            arrive(rs_in.at[d - 1, part], rs_s.at[b, d], rs_r.at[b, d])
        for k in range(lo, hi):
            total = after[own_rows, feat(k)] + own_sum[k, blk(x), :]
            for d in range(1, X):
                total = total + rs_in[d - 1, k].astype(F32)
            ag[c, x, k] = total.astype(BF16)
        ref = ag.at[c, x, part]
        for d in range(1, X):
            send(ref, ref, gx_s.at[b, d], gx_r.at[b, d], dev(x=xi(d)))
        send(ref, ref, gc_s.at[b, 0], gc_r.at[b, 0], dev(c=1 - c))

    def collect(b):
        lo, hi = cuts[b]
        part = pl.ds(lo, hi - lo)
        for d in range(1, X):
            ref = ag.at[c, xi(-d), part]
            arrive(ref, gx_s.at[b, d], gx_r.at[b, d])
            send(ref, ref, gc_s.at[b, d], gc_r.at[b, d], dev(c=1 - c))

    def unpack(b):
        lo, hi = cuts[b]
        part = pl.ds(lo, hi - lo)
        for d in range(0, X):
            arrive(ag.at[1 - c, xi(-d), part], gc_s.at[b, d], gc_r.at[b, d])
        for k in range(lo, hi):
            for ck in range(C):
                for xk in range(X):
                    r = ck * 128 + xk * 32
                    out[r : r + 32, feat(k)] = ag[ck, xk, k]

    def call(f, *a):
        return lambda: f(*a)

    stages = {
        0: [stage_zsend],
        2: [stage_zgroup],
        4: [stage_z],
        5: [stage_heads, stage_wout],
        6: [stage_heads2],
        7: [stage_wout2, stage_gathered, call(stage_project, 0, 4)],
        8: [call(stage_project, 4, 8), stage_norm],
        9: [stage_up, call(down, 0), call(down, 1), call(scatter, 0)],
    }

    pending = {0: [(0, z)], 1: [(0, z)]}
    ended = {0: [], 1: []}
    marks = [0]
    for t in range(0, STEPS + LAG + 2):
        for u, s in ((0, t), (1, t - LAG)):
            fresh = []
            for i in range(2):
                if 1 <= s + 1 <= STEPS - i:
                    step = s + 1
                    zk = zi((2 * i - 1) * step)
                    ref = wb.at[u, rows32(zk, y)]
                    arrive(ref, b1_s.at[i, u, step], b1_r.at[i, u, step])
                    if step + 1 <= STEPS - i:
                        send_b(u, i, step + 1, zk)
                    k = 2 * step - 1 + i
                    send_y(u, k, zk)
                    fresh.append((k, zk))
            for j in range(1):
                for i in range(2):
                    if 1 <= s <= STEPS - i:
                        zk = zi((2 * i - 1) * s)
                        ref = wa.at[u, group(zk)]
                        arrive(ref, a2_s.at[i, u, s, j], a2_r.at[i, u, s, j])
                        if s + 1 <= STEPS - i:
                            send_a(u, i, s + 1, zk, j)
            for k, zk in pending[u]:
                relay_y(u, k, zk)
            for k, zk in ended[u]:
                end_y(u, k, zk)
            ended[u], pending[u] = pending[u], fresh
        for stage in stages.get(t, []):
            stage()
        marks.append(len(sent))
        if len(marks) > 2:
            lo, hi = marks[-3], marks[-2]
            for cp in sent[lo:hi]:
                cp.wait_send()
    down(2)
    scatter(1)
    finish(0)
    scatter(2)
    finish(1)
    collect(0)
    finish(2)
    collect(1)
    unpack(0)
    collect(2)
    unpack(1)
    unpack(2)
    for cp in sent[marks[-2] :]:
        cp.wait_send()
    for d in range(1, Z // G):

        @pl.when(grp + d < Z // G)
        def _():
            rdma(gsend, gbuf.at[grp], gs_s.at[d], gs_r.at[d], dev(z=zi(d * G))).wait_send()


def body(
    resid,
    read_pre,
    keep_pre,
    written,
    emit_pre,
    shrink,
    floor_c,
    head_gain,
    wout,
    norm_gain,
    up,
    down,
):
    vm = pl.BlockSpec(memory_space=pltpu.VMEM)
    hbm = pl.BlockSpec(memory_space=pltpu.HBM)
    dma = pltpu.SemaphoreType.DMA
    call = pl.pallas_call(
        kernel,
        out_shape=jax.ShapeDtypeStruct((ROWS, D), BF16),
        in_specs=[hbm] * 12,
        out_specs=vm,
        scratch_shapes=[
            pltpu.VMEM((2, D, NA), BF16),
            pltpu.VMEM((2, D, NB), BF16),
            pltpu.VMEM((MIX, D), BF16),
            pltpu.VMEM((ROWS, HEAD), BF16),
            pltpu.VMEM((ROWS, HEAD), BF16),
            pltpu.VMEM((ROWS, HEAD), BF16),
            pltpu.VMEM((ROWS, HEAD), BF16),
            pltpu.VMEM((ROWS, HEAD), F32),
            pltpu.VMEM((1, HEAD), F32),
            pltpu.VMEM((1, HEAD), F32),
            pltpu.VMEM((1, D), F32),
            pltpu.VMEM((ROWS, D), BF16),
            pltpu.VMEM((ROWS, D), F32),
            pltpu.VMEM((ROWS, 1), F32),
            pltpu.VMEM((ROWS, D), BF16),
            pltpu.VMEM((ROWS, NA), BF16),
            pltpu.VMEM((ROWS, NB), BF16),
            pltpu.VMEM((ROWS, MIX), BF16),
            pltpu.VMEM((ROWS, HEAD), F32),
            pltpu.VMEM((ROWS, HEAD), F32),
            pltpu.VMEM((ROWS, HEAD), BF16),
            pltpu.VMEM((Y, HEAD + 16, HEAD), BF16),
            pltpu.VMEM((HEAD // Y + 16, HEAD), BF16),
            pltpu.VMEM((G, HEAD // Y + 16, HEAD), BF16),
            pltpu.VMEM((HEAD // Y + 16, HEAD), BF16),
            pltpu.VMEM((Z // G, HEAD // Y + 16, HEAD), BF16),
            pltpu.VMEM((HEAD, HEAD), F32),
            pltpu.VMEM((Z, 128, HEAD), BF16),
            pltpu.VMEM((Z, 128, HEAD), BF16),
            pltpu.VMEM((Z, 128, HEAD), F32),
            pltpu.VMEM((X - 1, Z, 32, HEAD), BF16),
            pltpu.VMEM((X - 1, Z, 32, HEAD), BF16),
            pltpu.VMEM((C, X, Z, 32, HEAD), BF16),
            pltpu.SemaphoreType.REGULAR((3,)),
            dma((14,)),
            dma((2, Y)),
            dma((2, Y)),
            dma((2, 2, STEPS + 1, Y)),
            dma((2, 2, STEPS + 1, Y)),
            dma((2, 2, STEPS + 1)),
            dma((2, 2, STEPS + 1)),
            dma((2, 2, Z)),
            dma((2, 2, Z)),
            dma((2, 2, Z)),
            dma((2, 2, Z)),
            dma((Y,)),
            dma((Y,)),
            dma((G,)),
            dma((G,)),
            dma((Z // G,)),
            dma((Z // G,)),
            dma((Y,)),
            dma((Y,)),
            dma((4,)),
            dma((4,)),
            dma((5,)),
            dma((5,)),
            dma((X,)),
            dma((X,)),
            dma((X,)),
            dma((X,)),
            dma((NB_CUT,)),
            dma((NB_CUT,)),
            dma((NB_CUT, X)),
            dma((NB_CUT, X)),
            dma((NB_CUT, X)),
            dma((NB_CUT, X)),
            dma((NB_CUT, X)),
            dma((NB_CUT, X)),
        ],
        compiler_params=pltpu.CompilerParams(
            collective_id=0, has_side_effects=True, vmem_limit_bytes=60 * 1024 * 1024
        ),
        name="layer",
    )
    return call(
        resid,
        read_pre,
        keep_pre,
        written,
        emit_pre,
        shrink,
        floor_c.reshape(1, -1),
        head_gain.reshape(1, -1),
        wout,
        norm_gain.reshape(1, -1),
        up,
        down,
    )


def solution(mesh):
    finer = Mesh(mesh.devices.reshape(Z, Y, X, C), ("z", "y", "x", "c"))
    sp, tp = ("z", "y"), ("x", "c")
    return jax.shard_map(
        body,
        mesh=finer,
        in_specs=(
            P(sp, None),
            P(sp, tp),
            P(sp, tp),
            P(sp, tp),
            P(sp, tp),
            P(sp, tp),
            P(tp),
            P(),
            P(tp, None),
            P(),
            P(sp, tp),
            P(sp, tp),
        ),
        out_specs=P(sp, None),
        check_vma=False,
    )
```

```python
import jax
import jax.numpy as jnp
from jax import lax
from jax.experimental import pallas as pl
from jax.experimental.pallas import tpu as pltpu
from jax.sharding import Mesh
from jax.sharding import PartitionSpec as P

Z, Y, X, C = 16, 4, 4, 2
HEAD = 128
BLOCK = 64
ROWS = 256
D = 2048
MIX = 1024
HID = 1024
NA = 384
NB = HID - NA
SP_N = Z * Y
WR = D // SP_N
G = 4
STEPS = Z // 2
LAG = 0
CUTS = (512, 1280, 2048)
NB_CUT = len(CUTS)
F32 = jnp.float32
BF16 = jnp.bfloat16
EPS = 1e-06
EXACT = lax.Precision.HIGHEST
NT = (((1,), (1,)), ((), ()))
TN = (((0,), (0,)), ((), ()))


def sigmoid(x):
    return 1.0 / (1.0 + jnp.exp(-x))


def log_one_minus(u):
    series = jnp.zeros_like(u)
    for k in range(9, 0, -1):
        series = u * (1.0 / k + series)
    return jnp.where(u < 0.125, -series, jnp.log(1.0 - u))


def one_minus_exp(w):
    series = jnp.ones_like(w)
    for k in range(10, 1, -1):
        series = 1.0 + (w * (1.0 / k)) * series
    return jnp.where(w > -0.5, -w * series, 1.0 - jnp.exp(w))


def kernel(
    resid_in,
    read_in,
    keep_in,
    written_in,
    emit_in,
    shrink_in,
    floor_in,
    head_gain_in,
    wout_in,
    norm_gain_in,
    up_in,
    down_in,
    out,
    wa,
    wb,
    wo,
    read_pre,
    keep_pre,
    written,
    emit_pre,
    shrink,
    floor_c,
    head_gain,
    norm_gain,
    resid,
    after,
    after_scale,
    normed,
    hid_a,
    hid_b,
    heads,
    local_out,
    q_decay,
    mixed,
    ybuf,
    zsend,
    zbuf,
    gsend,
    gbuf,
    pbuf,
    pair_out,
    pair_in,
    own_sum,
    rs_out,
    rs_in,
    acc,
    know,
    lsem,
    a1_s,
    a1_r,
    a2_s,
    a2_r,
    b1_s,
    b1_r,
    yf_s,
    yf_r,
    yh_s,
    yh_r,
    st_s,
    st_r,
    zs_s,
    zs_r,
    gs_s,
    gs_r,
    pq_s,
    pq_r,
    wx_s,
    wx_r,
    wc_s,
    wc_r,
    hx_s,
    hx_r,
    hc_s,
    hc_r,
    pp_s,
    pp_r,
    rs_s,
    rs_r,
    gx_s,
    gx_r,
    gc_s,
    gc_r,
):
    z = lax.axis_index("z")
    y = lax.axis_index("y")
    x = lax.axis_index("x")
    c = lax.axis_index("c")
    tp = x * C + c

    def zi(d):
        return lax.rem(z + (d + Z), Z)

    def yi(d):
        return lax.rem(y + (d + Y), Y)

    def xi(d):
        return lax.rem(x + (d + X), X)

    def dev(**kw):
        at = {"z": z, "y": y, "x": x, "c": c}
        at.update(kw)
        return (at["z"], at["y"], at["x"], at["c"])

    def rdma(src, dst, s, r, to):
        return pltpu.make_async_remote_copy(
            src_ref=src,
            dst_ref=dst,
            send_sem=s,
            recv_sem=r,
            device_id=to,
            device_id_type=pl.DeviceIdType.MESH,
        )

    sent = []

    def send(src, dst, s, r, to):
        cp = rdma(src, dst, s, r, to)
        cp.start()
        sent.append(cp)

    def arrive(ref, s, r):
        rdma(ref, ref, s, r, dev(c=1 - c)).wait_recv()

    bar = pltpu.get_barrier_semaphore()
    peers = [dev(z=zi(d)) for d in (1, Z - 1)]
    peers += [dev(y=yi(d)) for d in range(1, Y)]
    peers += [dev(x=xi(d)) for d in range(1, X)]
    peers += [dev(c=1 - c)]
    for p in peers:
        pl.semaphore_signal(bar, inc=1, device_id=p, device_id_type=pl.DeviceIdType.MESH)

    def rows32(zk, yk, n=WR, off=0):
        return pl.ds(pl.multiple_of((zk * Y + yk) * WR + off, 16), n)

    def a_own():
        return rows32(z, y)

    local = []
    for u, src in ((0, up_in), (1, down_in)):
        local.append(
            pltpu.make_async_copy(src.at[:, pl.ds(0, NA)], wa.at[u, a_own()], lsem.at[2 * u])
        )
        local.append(
            pltpu.make_async_copy(src.at[:, pl.ds(NA, NB)], wb.at[u, a_own()], lsem.at[2 * u + 1])
        )

    def orows(xk, ck, n=HEAD, off=0):
        return pl.ds(pl.multiple_of((xk * C + ck) * HEAD + off, 64), n)

    local.append(pltpu.make_async_copy(wout_in, wo.at[orows(x, c)], lsem.at[4]))
    for cp in local:
        cp.start()
    small = []
    for src, dst in (
        (floor_in, floor_c),
        (keep_in, keep_pre),
        (shrink_in, shrink),
        (read_in, read_pre),
        (written_in, written),
        (emit_in, emit_pre),
        (head_gain_in, head_gain),
        (norm_gain_in, norm_gain),
    ):
        small.append(pltpu.make_async_copy(src, dst, lsem.at[6 + len(small)]))
    for cp in small:
        cp.start()
    resid_copy = pltpu.make_async_copy(resid_in, resid, lsem.at[5])
    resid_copy.start()

    for cp in local:
        cp.wait()
    pl.semaphore_wait(bar, len(peers))

    def tell(n):
        for d in (1 << n, Z - (1 << n)):
            pl.semaphore_signal(
                know.at[n], inc=1, device_id=dev(z=zi(d)), device_id_type=pl.DeviceIdType.MESH
            )

    tell(0)
    def send_b(u, i, step, zk):
        ref = wb.at[u, rows32(zk, y)]
        send(ref, ref, b1_s.at[i, u, step], b1_r.at[i, u, step], dev(z=zi(1 - 2 * i)))

    def send_y(u, k, zk):
        ref = wb.at[u, rows32(zk, y)]
        for i in range(2):
            send(ref, ref, yf_s.at[i, u, k], yf_r.at[i, u, k], dev(y=yi(1 - 2 * i)))

    def relay_y(u, k, zk):
        for i in range(2):
            yk = yi(2 * i - 1)
            arrive(wb.at[u, rows32(zk, yk)], yf_s.at[i, u, k], yf_r.at[i, u, k])
            ref = wb.at[u, rows32(zk, yk, 16, 16 * i)]
            send(ref, ref, yh_s.at[i, u, k], yh_r.at[i, u, k], dev(y=yi(1 - 2 * i)))

    def end_y(u, k, zk):
        for i in range(2):
            ref = wb.at[u, rows32(zk, yi(2), 16, 16 * i)]
            arrive(ref, yh_s.at[i, u, k], yh_r.at[i, u, k])

    def group(zk):
        return pl.ds(pl.multiple_of(zk * (Y * WR), Y * WR), Y * WR)

    def send_a(u, i, step, zk, j):
        ref = wa.at[u, group(zk)]
        send(ref, ref, a2_s.at[i, u, step, j], a2_r.at[i, u, step, j], dev(z=zi(1 - 2 * i)))

    for i in range(2):
        send_b(0, i, 1, z)
    for u in range(2):
        for d in range(1, Y):
            ref = wa.at[u, a_own()]
            send(ref, ref, a1_s.at[u, d], a1_r.at[u, d], dev(y=yi(d)))
    for u in range(2):
        send_y(u, 0, z)
    own_wo = wo.at[orows(x, c)]
    for i in range(2):
        send(own_wo, own_wo, wx_s.at[i], wx_r.at[i], dev(x=xi(1 - 2 * i)))
    send(own_wo, own_wo, wc_s.at[0], wc_r.at[0], dev(c=1 - c))

    for cp in small:
        cp.wait()
    floor = floor_c[...]
    pre = keep_pre[...].astype(F32)
    logs = log_one_minus(floor * (1.0 / (1.0 + jnp.exp(pre)))) + shrink[...]
    key = one_minus_exp(logs)
    rp = read_pre[...].astype(F32)
    query = rp * sigmoid(rp)
    value = written[...].astype(F32)
    ti = lax.broadcasted_iota(jnp.int32, (BLOCK, BLOCK), 0)
    si = lax.broadcasted_iota(jnp.int32, (BLOCK, BLOCK), 1)
    lower = ti >= si
    tri = lower.astype(F32)
    state = jnp.zeros((HEAD, HEAD), F32)
    base = jnp.zeros((1, HEAD), F32)
    parts = []
    for k in range(ROWS // BLOCK):
        sl = slice(k * BLOCK, (k + 1) * BLOCK)
        lc = jnp.dot(tri, logs[sl], precision=EXACT, preferred_element_type=F32)
        end = lc[BLOCK - 1 :, :]
        kd = key[sl] * jnp.exp(end - lc)
        parts.append((sl, lc, state))
        q_decay[sl, :] = query[sl] * jnp.exp(lc + base)
        state = jnp.exp(end) * state + lax.dot_general(
            value[sl], kd, TN, precision=EXACT, preferred_element_type=F32
        )
        base = base + end
    decay = jnp.exp(base)

    def two_parts(a):
        hi = a.astype(BF16)
        lo = (a - hi.astype(F32)).astype(BF16)
        r = lax.broadcasted_iota(jnp.int32, (16, HEAD), 0)
        both = jnp.where(r == 0, hi.astype(F32), jnp.where(r == 1, lo.astype(F32), 0.0))
        return both.astype(BF16)

    ybuf[y, 0:HEAD, :] = state.astype(BF16)
    ybuf[y, HEAD : HEAD + 16, :] = two_parts(decay)

    for d in range(1, Y):
        send(ybuf.at[y], ybuf.at[y], st_s.at[d], st_r.at[d], dev(y=yi(d)))

    for sl, lc, st in parts:
        qd = query[sl] * jnp.exp(lc)
        kd = key[sl] * jnp.exp(-lc)
        scores = lax.dot_general(qd, kd, NT, precision=EXACT, preferred_element_type=F32)
        scores = jnp.where(lower, scores, 0.0)
        local_out[sl, :] = jnp.dot(
            scores, value[sl], precision=EXACT, preferred_element_type=F32
        ) + lax.dot_general(qd, st, NT, precision=EXACT, preferred_element_type=F32)

    pl.semaphore_wait(know.at[0], 2)
    tell(1)
    for u in range(2):
        for d in range(1, Y):
            arrive(wa.at[u, rows32(z, yi(-d))], a1_s.at[u, d], a1_r.at[u, d])
        if u == 0:
            for i in range(2):
                send_a(0, i, 1, z, 0)
    for i in range(2):
        send_b(1, i, 1, z)
    for i in range(2):
        send_a(1, i, 1, z, 0)

    def decay_of(block):
        return block[0:1, :].astype(F32) + block[1:2, :].astype(F32)

    for d in range(1, Y):
        arrive(ybuf.at[yi(-d)], st_s.at[d], st_r.at[d])
    quarter = pl.ds(pl.multiple_of(y * (HEAD // Y), HEAD // Y), HEAD // Y)
    row_q = jnp.zeros((HEAD // Y, HEAD), F32)
    row_a = jnp.ones((1, HEAD), F32)
    for k in range(Y):
        a_k = decay_of(ybuf[k, HEAD : HEAD + 16, :])
        row_q = a_k * row_q + ybuf[k, quarter, :].astype(F32)
        row_a = row_a * a_k
    zsend[0 : HEAD // Y, :] = row_q.astype(BF16)
    zsend[HEAD // Y : HEAD // Y + 16, :] = two_parts(row_a)

    grp = z // G
    inner = z % G

    def zg(d):
        return grp * G + lax.rem(inner + (d + G), G)

    def stage_zsend():
        pl.semaphore_wait(know.at[1], 2)
        tell(2)
        for d in range(1, G):
            send(zsend, zbuf.at[inner], zs_s.at[d], zs_r.at[d], dev(z=zg(d)))

    def decay_rows(ref, k):
        return decay_of(ref[k, HEAD // Y : HEAD // Y + 16, :])

    def stage_zgroup():
        for d in range(1, G):
            arrive(zbuf.at[lax.rem(inner + (G - d), G)], zs_s.at[d], zs_r.at[d])
        zbuf[inner] = zsend[...]
        pl.semaphore_wait(know.at[2], 2)
        total = jnp.zeros((HEAD // Y, HEAD), F32)
        total_a = jnp.ones((1, HEAD), F32)
        for k in range(G):
            a_k = decay_rows(zbuf, k)
            total = a_k * total + zbuf[k, 0 : HEAD // Y, :].astype(F32)
            total_a = total_a * a_k
        gsend[0 : HEAD // Y, :] = total.astype(BF16)
        gsend[HEAD // Y : HEAD // Y + 16, :] = two_parts(total_a)
        for d in range(1, Z // G):

            @pl.when(grp + d < Z // G)
            def _():
                rdma(gsend, gbuf.at[grp], gs_s.at[d], gs_r.at[d], dev(z=zi(d * G))).start()

    def stage_wout():
        for i in range(2):
            xk = xi(2 * i - 1)
            full = wo.at[orows(xk, c)]
            arrive(full, wx_s.at[i], wx_r.at[i])
            half = wo.at[orows(xk, c, 64, 64 * i)]
            send(half, half, wx_s.at[2 + i], wx_r.at[2 + i], dev(x=xi(1 - 2 * i)))
            send(full, full, wc_s.at[1 + i], wc_r.at[1 + i], dev(c=1 - c))

    def stage_wout2():
        for i in range(2):
            half = wo.at[orows(xi(2), c, 64, 64 * i)]
            arrive(half, wx_s.at[2 + i], wx_r.at[2 + i])
            send(half, half, wc_s.at[3 + i], wc_r.at[3 + i], dev(c=1 - c))

    def stage_z():
        for d in range(1, Z // G):

            @pl.when(grp - d >= 0)
            def _():
                arrive(gbuf.at[grp - d], gs_s.at[d], gs_r.at[d])

        def add(k, acc):
            return decay_rows(gbuf, k) * acc + gbuf[k, 0 : HEAD // Y, :].astype(F32)

        def add_in(k, acc):
            return decay_rows(zbuf, k) * acc + zbuf[k, 0 : HEAD // Y, :].astype(F32)

        before = lax.fori_loop(0, grp, add, jnp.zeros((HEAD // Y, HEAD), F32))
        pbuf[quarter, :] = lax.fori_loop(0, inner, add_in, before)
        for d in range(1, Y):
            ref = pbuf.at[quarter]
            send(ref, ref, pq_s.at[d], pq_r.at[d], dev(y=yi(d)))

    def stage_heads():
        for d in range(1, Y):
            there = pl.ds(pl.multiple_of(yi(-d) * (HEAD // Y), HEAD // Y), HEAD // Y)
            arrive(pbuf.at[there], pq_s.at[d], pq_r.at[d])
        prior = pbuf[...]
        for k in range(Y - 1):
            a_k = decay_of(ybuf[k, HEAD : HEAD + 16, :])
            prior = jnp.where(k < y, a_k * prior + ybuf[k, 0:HEAD, :].astype(F32), prior)
        recur = local_out[...] + lax.dot_general(
            q_decay[...], prior, NT, precision=EXACT, preferred_element_type=F32
        )
        ep = emit_pre[...].astype(F32)
        norm = lax.rsqrt(jnp.mean(recur * recur, axis=-1, keepdims=True) + EPS)
        mixed[...] = (recur * norm * head_gain[...] * (ep * sigmoid(ep))).astype(BF16)
        heads[:, cols(x, c)] = mixed[...]
        dst = heads.at[:, cols(x, c)]
        for d in range(1, X):
            send(mixed, dst, hx_s.at[d], hx_r.at[d], dev(x=xi(d)))
        send(mixed, dst, hc_s.at[0], hc_r.at[0], dev(c=1 - c))

    def cols(xk, ck):
        return pl.ds(pl.multiple_of((xk * C + ck) * HEAD, HEAD), HEAD)

    def stage_heads2():
        for d in range(1, X):
            ref = heads.at[:, cols(xi(-d), c)]
            arrive(ref, hx_s.at[d], hx_r.at[d])
            send(ref, ref, hc_s.at[d], hc_r.at[d], dev(c=1 - c))

    tile = 256

    def stage_gathered():
        for i in range(2):
            arrive(wo.at[orows(xi(2 * i - 1), 1 - c)], wc_s.at[1 + i], wc_r.at[1 + i])
            arrive(wo.at[orows(xi(2), 1 - c, 64, 64 * i)], wc_s.at[3 + i], wc_r.at[3 + i])
        arrive(wo.at[orows(x, 1 - c)], wc_s.at[0], wc_r.at[0])
        for d in range(0, X):
            arrive(heads.at[:, cols(xi(-d), 1 - c)], hc_s.at[d], hc_r.at[d])
        resid_copy.wait()
        after_scale[...] = jnp.zeros((ROWS, 1), F32)

    def stage_project(lo, hi):
        def project(n, square):
            at = pl.ds(pl.multiple_of(n * tile, tile), tile)
            got = resid[:, at].astype(F32) + jnp.dot(
                heads[...], wo[:, at], preferred_element_type=F32
            )
            after[:, at] = got
            return square + jnp.sum(got * got, axis=-1, keepdims=True)

        after_scale[...] = lax.fori_loop(lo, hi, project, after_scale[...])

    def stage_norm():
        after_scale[...] = lax.rsqrt(after_scale[...] * (1.0 / D) + EPS)

        def scaled(n, carry):
            at = pl.ds(pl.multiple_of(n * tile, tile), tile)
            for j in range(2):
                half = pl.ds(pl.multiple_of(jnp.where(j == 0, 1 - c, c) * 128, 128), 128)
                normed[128 * j : 128 * (j + 1), at] = (
                    after[half, at] * after_scale[half, :] * norm_gain[:, at]
                ).astype(BF16)
            return carry

        lax.fori_loop(0, D // tile, scaled, 0)

    def zk_of(k):
        return zi(k // 2 if k % 2 == 0 else -(k + 1) // 2)

    tiles = [(buf, w, at, min(256, n - at)) for buf, w, n in ((hid_a, wa, NA), (hid_b, wb, NB))
             for at in range(0, n, 256)]

    def partial_up(w, at, n, ks):
        total = jnp.zeros((ROWS, n), F32)
        for k in ks:
            fr = group(zk_of(k))
            total += jnp.dot(normed[:, fr], w[0, fr, at : at + n], preferred_element_type=F32)
        return total

    def stage_up_most():
        for q, (_, w, at, n) in enumerate(tiles):
            acc[q, :, 0:n] = partial_up(w, at, n, range(Z - 1))

    def stage_up():
        for q, (buf, w, at, n) in enumerate(tiles):
            h = acc[q, :, 0:n] + partial_up(w, at, n, [Z - 1])
            h = jnp.maximum(h, 0.0)
            buf[:, at : at + n] = (h * h).astype(BF16)

    def blk(xk):
        return pl.ds(pl.multiple_of(xk * 32, 32), 32)

    def orow(xk, ck):
        return pl.ds(pl.multiple_of(ck * 128 + xk * 32, 32), 32)

    own_rows = orow(x, c)
    spans = [(0 if b == 0 else CUTS[b - 1], CUTS[b]) for b in range(NB_CUT)]

    def down(b):
        lo, hi = spans[b]
        for f in range(lo, hi, 256):
            at = slice(f, f + 256)
            got = lax.dot_general(hid_a[...], wa[1, at, :], NT, preferred_element_type=F32)
            got += lax.dot_general(hid_b[...], wb[1, at, :], NT, preferred_element_type=F32)
            pair_out[:, at] = got[0:128].astype(BF16)
            own_sum[:, at] = got[128:256]
        part = pl.ds(lo, hi - lo)
        send(pair_out.at[:, part], pair_in.at[:, part], pp_s.at[b], pp_r.at[b], dev(c=1 - c))

    def scatter(b):
        lo, hi = spans[b]
        part = pl.ds(lo, hi - lo)
        arrive(pair_in.at[:, part], pp_s.at[b], pp_r.at[b])
        own_sum[:, lo:hi] = own_sum[:, lo:hi] + pair_in[:, lo:hi].astype(F32)
        for d in (2, 1, 3):
            rs_out[d - 1, :, lo:hi] = own_sum[blk(xi(d)), lo:hi].astype(BF16)
            src, dst = rs_out.at[d - 1, :, part], rs_in.at[d - 1, :, part]
            send(src, dst, rs_s.at[b, d], rs_r.at[b, d], dev(x=xi(d)))

    def finish(b):
        lo, hi = spans[b]
        part = pl.ds(lo, hi - lo)
        for d in range(1, X):
            arrive(rs_in.at[d - 1, :, part], rs_s.at[b, d], rs_r.at[b, d])
        total = after[own_rows, lo:hi] + own_sum[blk(x), lo:hi]
        for d in range(1, X):
            total = total + rs_in[d - 1, :, lo:hi].astype(F32)
        out[own_rows, lo:hi] = total.astype(BF16)
        ref = out.at[own_rows, part]
        for d in (2, 1, 3):
            send(ref, ref, gx_s.at[b, d], gx_r.at[b, d], dev(x=xi(d)))
        send(ref, ref, gc_s.at[b, 0], gc_r.at[b, 0], dev(c=1 - c))

    def collect(b):
        lo, hi = spans[b]
        part = pl.ds(lo, hi - lo)
        for d in (1, 3, 2):
            ref = out.at[orow(xi(-d), c), part]
            arrive(ref, gx_s.at[b, d], gx_r.at[b, d])
            send(ref, ref, gc_s.at[b, d], gc_r.at[b, d], dev(c=1 - c))

    def ended_batch(b):
        lo, hi = spans[b]
        part = pl.ds(lo, hi - lo)
        for d in range(0, X):
            arrive(out.at[orow(xi(-d), 1 - c), part], gc_s.at[b, d], gc_r.at[b, d])

    def call(f, *a):
        return lambda: f(*a)

    stages = {
        0: [stage_zsend],
        1: [stage_zgroup],
        3: [stage_z],
        4: [stage_heads, stage_wout],
        5: [stage_heads2, stage_wout2],
        6: [stage_gathered, call(stage_project, 0, 4)],
        7: [call(stage_project, 4, 8), stage_norm],
        8: [stage_up_most],
        9: [stage_up],
    }

    pending = {0: [(0, z)], 1: [(0, z)]}
    ended = {0: [], 1: []}
    marks = [0]
    for t in range(0, STEPS + LAG + 2):
        for u, s in ((0, t), (1, t - LAG)):
            fresh = []
            for i in range(2):
                if 1 <= s + 1 <= STEPS - i:
                    step = s + 1
                    zk = zi((2 * i - 1) * step)
                    ref = wb.at[u, rows32(zk, y)]
                    arrive(ref, b1_s.at[i, u, step], b1_r.at[i, u, step])
                    if step + 1 <= STEPS - i:
                        send_b(u, i, step + 1, zk)
                    k = 2 * step - 1 + i
                    send_y(u, k, zk)
                    fresh.append((k, zk))
            for k, zk in pending[u]:
                relay_y(u, k, zk)
            for k, zk in ended[u]:
                end_y(u, k, zk)
            for j in range(1):
                for i in range(2):
                    if 1 <= s <= STEPS - i:
                        zk = zi((2 * i - 1) * s)
                        ref = wa.at[u, group(zk)]
                        arrive(ref, a2_s.at[i, u, s, j], a2_r.at[i, u, s, j])
                        if s + 1 <= STEPS - i:
                            send_a(u, i, s + 1, zk, j)
            ended[u], pending[u] = pending[u], fresh
        for stage in stages.get(t, []):
            stage()
        marks.append(len(sent))
        if len(marks) > 2:
            lo, hi = marks[-3], marks[-2]
            for cp in sent[lo:hi]:
                cp.wait_send()
    for b in range(NB_CUT + 3):
        if b < NB_CUT:
            down(b)
        if 1 <= b < NB_CUT + 1:
            scatter(b - 1)
        if 2 <= b < NB_CUT + 2:
            finish(b - 2)
        if 3 <= b:
            collect(b - 3)
    for b in range(NB_CUT):
        ended_batch(b)
    for cp in sent[marks[-2] :]:
        cp.wait_send()
    for d in range(1, Z // G):

        @pl.when(grp + d < Z // G)
        def _():
            rdma(gsend, gbuf.at[grp], gs_s.at[d], gs_r.at[d], dev(z=zi(d * G))).wait_send()


def body(
    resid,
    read_pre,
    keep_pre,
    written,
    emit_pre,
    shrink,
    floor_c,
    head_gain,
    wout,
    norm_gain,
    up,
    down,
):
    vm = pl.BlockSpec(memory_space=pltpu.VMEM)
    hbm = pl.BlockSpec(memory_space=pltpu.HBM)
    dma = pltpu.SemaphoreType.DMA
    call = pl.pallas_call(
        kernel,
        out_shape=jax.ShapeDtypeStruct((ROWS, D), BF16),
        in_specs=[hbm] * 12,
        out_specs=vm,
        scratch_shapes=[
            pltpu.VMEM((2, D, NA), BF16),
            pltpu.VMEM((2, D, NB), BF16),
            pltpu.VMEM((MIX, D), BF16),
            pltpu.VMEM((ROWS, HEAD), BF16),
            pltpu.VMEM((ROWS, HEAD), BF16),
            pltpu.VMEM((ROWS, HEAD), BF16),
            pltpu.VMEM((ROWS, HEAD), BF16),
            pltpu.VMEM((ROWS, HEAD), F32),
            pltpu.VMEM((1, HEAD), F32),
            pltpu.VMEM((1, HEAD), F32),
            pltpu.VMEM((1, D), F32),
            pltpu.VMEM((ROWS, D), BF16),
            pltpu.VMEM((ROWS, D), F32),
            pltpu.VMEM((ROWS, 1), F32),
            pltpu.VMEM((ROWS, D), BF16),
            pltpu.VMEM((ROWS, NA), BF16),
            pltpu.VMEM((ROWS, NB), BF16),
            pltpu.VMEM((ROWS, MIX), BF16),
            pltpu.VMEM((ROWS, HEAD), F32),
            pltpu.VMEM((ROWS, HEAD), F32),
            pltpu.VMEM((ROWS, HEAD), BF16),
            pltpu.VMEM((Y, HEAD + 16, HEAD), BF16),
            pltpu.VMEM((HEAD // Y + 16, HEAD), BF16),
            pltpu.VMEM((G, HEAD // Y + 16, HEAD), BF16),
            pltpu.VMEM((HEAD // Y + 16, HEAD), BF16),
            pltpu.VMEM((Z // G, HEAD // Y + 16, HEAD), BF16),
            pltpu.VMEM((HEAD, HEAD), F32),
            pltpu.VMEM((128, D), BF16),
            pltpu.VMEM((128, D), BF16),
            pltpu.VMEM((128, D), F32),
            pltpu.VMEM((X - 1, 32, D), BF16),
            pltpu.VMEM((X - 1, 32, D), BF16),
            pltpu.VMEM((5, ROWS, 256), F32),
            pltpu.SemaphoreType.REGULAR((3,)),
            dma((14,)),
            dma((2, Y)),
            dma((2, Y)),
            dma((2, 2, STEPS + 1, Y)),
            dma((2, 2, STEPS + 1, Y)),
            dma((2, 2, STEPS + 1)),
            dma((2, 2, STEPS + 1)),
            dma((2, 2, Z)),
            dma((2, 2, Z)),
            dma((2, 2, Z)),
            dma((2, 2, Z)),
            dma((Y,)),
            dma((Y,)),
            dma((G,)),
            dma((G,)),
            dma((Z // G,)),
            dma((Z // G,)),
            dma((Y,)),
            dma((Y,)),
            dma((4,)),
            dma((4,)),
            dma((5,)),
            dma((5,)),
            dma((X,)),
            dma((X,)),
            dma((X,)),
            dma((X,)),
            dma((NB_CUT,)),
            dma((NB_CUT,)),
            dma((NB_CUT, X)),
            dma((NB_CUT, X)),
            dma((NB_CUT, X)),
            dma((NB_CUT, X)),
            dma((NB_CUT, X)),
            dma((NB_CUT, X)),
        ],
        compiler_params=pltpu.CompilerParams(
            collective_id=0, has_side_effects=True, vmem_limit_bytes=60 * 1024 * 1024
        ),
        name="layer",
    )
    return call(
        resid,
        read_pre,
        keep_pre,
        written,
        emit_pre,
        shrink,
        floor_c.reshape(1, -1),
        head_gain.reshape(1, -1),
        wout,
        norm_gain.reshape(1, -1),
        up,
        down,
    )


def solution(mesh):
    finer = Mesh(mesh.devices.reshape(Z, Y, X, C), ("z", "y", "x", "c"))
    sp, tp = ("z", "y"), ("x", "c")
    return jax.shard_map(
        body,
        mesh=finer,
        in_specs=(
            P(sp, None),
            P(sp, tp),
            P(sp, tp),
            P(sp, tp),
            P(sp, tp),
            P(sp, tp),
            P(tp),
            P(),
            P(tp, None),
            P(),
            P(sp, tp),
            P(sp, tp),
        ),
        out_specs=P(sp, None),
        check_vma=False,
    )
```
